32 devices in a mesh: sp: 16 (over z, y, x), tp: 2 (over core).
Axes of the slice: x: 2, y: 2, z: 4, core: 2. Of those that a mesh axis runs over, the one named last changes fastest.
Arguments:
- tokens: bfloat16 [4096, 2048], P('sp'), may hold values from -6 to 6
- input_norm_gain: float32 [2048], replicated, may hold values from 0.1 to 1.9
- mq_weight: bfloat16 [2048, 1024], P('sp', 'tp'), may hold values from -0.125 to 0.125
- mk_weight: bfloat16 [2048, 1024], P('sp', 'tp'), may hold values from -0.125 to 0.125
- mv_weight: bfloat16 [2048, 1024], P('sp', 'tp'), may hold values from -0.125 to 0.125
- mo_weight: bfloat16 [2048, 1024], P('sp', 'tp'), may hold values from -0.125 to 0.125
- gate_weight: bfloat16 [2048, 4, 8], P('sp', None, 'tp'), may hold values from -0.125 to 0.125
- gate_bias: float32 [4, 8], P(None, 'tp'), may hold values from -3 to 100
- decay_extra: float32 [2, 8, 4096], P(None, 'tp', 'sp'), may hold values from -1 to 0
- m_gain: float32 [1024], P('tp'), may hold values from 0.1 to 1.9
- aq_weight: bfloat16 [2048, 1024], P('sp', 'tp'), may hold values from -0.125 to 0.125
- ak_weight: bfloat16 [2048, 512], P('sp', 'tp'), may hold values from -8.838835 to 8.838835
- av_weight: bfloat16 [2048, 512], P('sp', 'tp'), may hold values from -0.125 to 0.125
- sink_logit: float32 [16], P('tp'), may hold values from 3 to 6
- out_m_weight: bfloat16 [1024, 2048], P('sp', 'tp'), may hold values from -0.1875 to 0.1875
- out_a_weight: bfloat16 [1024, 2048], P('sp', 'tp'), may hold values from -1.5 to 1.5
Outputs:
- mixed: bfloat16 [4096, 2048], P('sp', 'tp')
- log_total: float32 [16, 4096], P('tp', 'sp')
The draws below stay inside these ranges and needn't reach their ends.
All inputs are finite; a program needn't handle non-finite values.
Results may differ from the reference program's by a relative error of at most 0.015.
The reference program's roundings to bfloat16 on the way count: a program that leaves them out, or rounds other values in their place, can miss the bound.
Values may be sent and summed in bfloat16 or wider, within the bound.
A program may use at most 64 MiB of HBM per device.

```python
import math
import jax
import jax.numpy as jnp
from jax import lax

D = 2048
M_HEADS = 8
M_DIM = 128
W_HEADS = 16
KEY_VALUE_HEADS = 8
W_DIM = 64
WINDOW = 128
M_BLOCK = 64
TOK_DEV = 256
SEQUENCE_STEPS = 4096
M_WIDTH = 1024
W_WIDTH = 1024
KV_WIDTH = 512


def draw_gate_bias(key, part):
    keys_all = jax.random.split(jax.random.fold_in(key, 11), 4)
    inputs_gate = jax.random.truncated_normal(keys_all[0], -3.0, 3.0, (2, M_HEADS), jnp.float32)
    fast_share = 0.5
    fast_heads = jax.random.uniform(keys_all[1], (2, M_HEADS), jnp.float32) < fast_share
    fast_value = jax.random.uniform(keys_all[2], (2, M_HEADS), jnp.float32, 2.5, 3.5)
    slow_value = math.log(SEQUENCE_STEPS) + jax.random.uniform(keys_all[3], (2, M_HEADS), jnp.float32, 1.0, 2.0)
    forget_bias = jnp.where(fast_heads, fast_value, slow_value)
    return jnp.stack([inputs_gate[0], forget_bias[0], inputs_gate[1], forget_bias[1]])


def draw_decay_extra(key, part):
    keys_all = jax.random.split(jax.random.fold_in(key, 23), 3)
    block_total = SEQUENCE_STEPS // TOK_DEV
    rates = jnp.exp(jax.random.uniform(keys_all[0], (2, M_HEADS, block_total), jnp.float32, math.log(0.2), math.log(2.0))) / SEQUENCE_STEPS
    reference_speed = -jnp.repeat(rates, TOK_DEV, axis=2)
    spots = jax.random.randint(keys_all[1], (2, M_HEADS, 2), 0, SEQUENCE_STEPS)
    stacked_level = jnp.log(jax.random.uniform(keys_all[2], (2, M_HEADS, 2), jnp.float32, 0.5, 0.8))
    places = jnp.arange(SEQUENCE_STEPS, dtype=jnp.int32)
    equality_detected = places[None, None, :, None] == spots[:, :, None, :]
    clustered_spikes = jnp.sum(jnp.where(equality_detected, stacked_level[:, :, None, :], 0.0), axis=-1)
    return reference_speed + clustered_spikes


def draw_ak_weight(key, part):
    base_draw = jax.random.truncated_normal(jax.random.fold_in(key, 5), -4.0, 4.0, (D, KV_WIDTH), jnp.float32) * D ** (-0.5)
    return base_draw.astype(jnp.bfloat16)


def block_levels(key, extent, shards, smallest, high):
    gain = 1.0
    for dim, parts in shards:
        steps = jax.random.uniform(jax.random.fold_in(jax.random.fold_in(key, 6), dim), (parts,), jnp.float32, smallest / len(shards), high / len(shards))
        gain = gain * jnp.repeat(jnp.exp(steps), extent[dim] // parts).reshape((-1,) + (1,) * (len(extent) - 1 - dim))
    return gain


def centred(own_key, extent, deviation, bound, pieces=(), kind=jnp.bfloat16):
    loudness = block_levels(own_key, extent, pieces, -0.22, 0.18) if pieces else 1.0
    drawn = jax.random.normal(own_key, extent, jnp.float32) * deviation * loudness
    return jnp.minimum(jnp.maximum(drawn, -bound), bound).astype(kind)


def setup_inputs(seed: int = 0) -> dict:
    key_list = jax.random.split(jax.random.key(seed), 17)
    return {
        "tokens": centred(key_list[0], (SEQUENCE_STEPS, D), 1.0, 6.0, ((0, 16),)),
        "input_norm_gain": jnp.clip(1.0 + 0.18 * jax.random.normal(key_list[1], (D,), jnp.float32), 0.1, 1.9),
        "mq_weight": centred(key_list[2], (D, M_WIDTH), D ** -0.5, 0.125, ((0, 16), (1, 2))),
        "mk_weight": centred(key_list[3], (D, M_WIDTH), D ** -0.5, 0.125, ((0, 16), (1, 2))),
        "mv_weight": centred(key_list[4], (D, M_WIDTH), D ** -0.5, 0.125, ((0, 16), (1, 2))),
        "mo_weight": centred(key_list[5], (D, M_WIDTH), D ** -0.5, 0.125, ((0, 16), (1, 2))),
        "gate_weight": centred(key_list[6], (D, 4, M_HEADS), D ** -0.5, 0.125, ((0, 16), (2, 2))),
        "gate_bias": draw_gate_bias(jax.random.fold_in(key_list[16], 71), 0),
        "decay_extra": draw_decay_extra(jax.random.fold_in(key_list[16], 71), 0),
        "m_gain": jnp.clip(1.0 + 0.18 * jax.random.normal(key_list[9], (M_WIDTH,), jnp.float32), 0.1, 1.9),
        "aq_weight": centred(key_list[10], (D, W_WIDTH), D ** -0.5, 0.125, ((0, 16), (1, 2))),
        "ak_weight": draw_ak_weight(jax.random.fold_in(key_list[16], 71), 0),
        "av_weight": centred(key_list[12], (D, KV_WIDTH), D ** -0.5, 0.125, ((0, 16), (1, 2))),
        "sink_logit": jnp.clip(3.0 + 3.0 * jax.random.uniform(key_list[13], (W_HEADS,), jnp.float32) ** block_levels(key_list[13], (W_HEADS,), ((0, 2),), -0.2, 0.2), 3.0, 6.0),
        "out_m_weight": centred(key_list[14], (M_WIDTH, D), M_WIDTH ** -0.5, 0.1875, ((0, 16), (1, 2))),
        "out_a_weight": centred(key_list[15], (W_WIDTH, D), (W_WIDTH // 64) ** -0.5, 1.5, ((0, 16), (1, 2))),
    }


EPS = 1e-06
HIGHEST = lax.Precision.HIGHEST

def rms_rows(inputs, gain_vec):
    return inputs * lax.rsqrt(lax.optimization_barrier(jnp.mean(inputs * inputs, axis=-1, keepdims=True)) + EPS) * gain_vec

def stored(result):
    return lax.optimization_barrier(result.astype(jnp.bfloat16))

def block_pass(queries, key_vecs, value_vecs, in_gate, log_forget, start_state):
    head_count, length, head_width = queries.shape
    block_count = length // M_BLOCK

    def blocks(array_in):
        return jnp.moveaxis(array_in.reshape((head_count, block_count, M_BLOCK) + array_in.shape[2:]), 1, 0)
    lower_mask = jnp.tril(jnp.ones((M_BLOCK, M_BLOCK), dtype=bool))

    def advance(state_in, block_in):
        cell_mat, norm_vec, stab_max = state_in
        q_blk, k_blk, v_blk, i_blk, f_blk = block_in
        cum_log = jnp.cumsum(f_blk, axis=-1)
        seg_total = cum_log[:, -1]
        log_end = seg_total[:, None] - cum_log + i_blk
        max_next = jnp.maximum(seg_total + stab_max, lax.optimization_barrier(jnp.max(log_end, axis=-1)))
        w_end = jnp.exp(log_end - max_next[:, None])
        fade_old = jnp.exp(seg_total + stab_max - max_next)
        cell_next = fade_old[:, None, None] * cell_mat + jnp.einsum('hsv,hsk->hvk', w_end[:, :, None] * v_blk, k_blk, precision=HIGHEST)
        norm_next = fade_old[:, None] * norm_vec + jnp.einsum('hs,hsk->hk', w_end, k_blk, precision=HIGHEST)
        log_w = jnp.where(lower_mask, cum_log[:, :, None] - cum_log[:, None, :] + i_blk[:, None, :], -jnp.inf)
        log_inter = cum_log + stab_max[:, None]
        row_max = jnp.maximum(log_inter, lax.optimization_barrier(jnp.max(log_w, axis=-1)))
        w_intra = jnp.exp(log_w - row_max[:, :, None])
        w_inter = jnp.exp(log_inter - row_max)
        scores = jnp.einsum('htk,hsk->hts', q_blk, k_blk, precision=HIGHEST) * w_intra
        numerator = jnp.einsum('hts,hsv->htv', scores, v_blk, precision=HIGHEST) + w_inter[..., None] * jnp.einsum('hvk,htk->htv', cell_mat, q_blk, precision=HIGHEST)
        denominator = lax.optimization_barrier(jnp.sum(scores, axis=-1)) + w_inter * jnp.einsum('hk,htk->ht', norm_vec, q_blk, precision=HIGHEST)
        result_rows = numerator / jnp.maximum(jnp.abs(denominator), jnp.exp(-row_max))[..., None]
        return ((cell_next, norm_next, max_next), result_rows)
    final_state, outputs = lax.scan(advance, start_state, tuple((blocks(array_in) for array_in in (queries, key_vecs, value_vecs, in_gate, log_forget))))
    return (jnp.moveaxis(outputs, 0, 1).reshape(head_count, length, head_width), final_state)

def flip_tokens(array_in):
    return jnp.flip(array_in, axis=1)

def window_attention(a_query, a_key, a_value, sink_logit):
    length = a_query.shape[0]
    block_count = length // WINDOW
    groups = W_HEADS // KEY_VALUE_HEADS
    query_blocks = a_query.reshape(block_count, WINDOW, KEY_VALUE_HEADS, groups, W_DIM)
    border = ((WINDOW, WINDOW), (0, 0))
    key_pad = jnp.pad(a_key, border).reshape(length + 2 * WINDOW, KEY_VALUE_HEADS, W_DIM)
    value_pad = jnp.pad(a_value, border).reshape(length + 2 * WINDOW, KEY_VALUE_HEADS, W_DIM)
    query_off = jnp.arange(WINDOW, dtype=jnp.int32)
    key_off = jnp.arange(3 * WINDOW, dtype=jnp.int32) - WINDOW
    in_window = jnp.abs(query_off[:, None] - key_off[None, :]) <= WINDOW
    sink_col = sink_logit.reshape(KEY_VALUE_HEADS, groups, 1)

    def one_block(block_in):
        index, query_rows = block_in
        first = (index * WINDOW).astype(jnp.int32)
        key_rows = lax.dynamic_slice_in_dim(key_pad, first, 3 * WINDOW, 0).astype(jnp.float32)
        value_rows = lax.dynamic_slice_in_dim(value_pad, first, 3 * WINDOW, 0).astype(jnp.float32)
        key_place = first + key_off
        usable = in_window & ((key_place >= 0) & (key_place < length))[None, :]
        scores = jnp.einsum('qgrd,kgd->grqk', query_rows.astype(jnp.float32), key_rows) * W_DIM ** (-0.5)
        scores = jnp.where(usable, scores, -jnp.inf)
        peak_log = jnp.maximum(sink_col, lax.optimization_barrier(jnp.max(scores, axis=-1)))
        weights_exp = jnp.exp(scores - peak_log[..., None])
        weight_total_sum = jnp.exp(sink_col - peak_log) + lax.optimization_barrier(jnp.sum(weights_exp, axis=-1))
        rounded = weights_exp.astype(jnp.bfloat16).astype(jnp.float32)
        weighted = jnp.einsum('grqk,kgd->qgrd', rounded, value_rows)
        mixed_rows = (weighted / jnp.transpose(weight_total_sum, (2, 0, 1))[..., None]).astype(jnp.bfloat16)
        return (mixed_rows.reshape(WINDOW, W_HEADS * W_DIM), (peak_log + jnp.log(weight_total_sum)).reshape(W_HEADS, WINDOW))
    mixed_blocks, log_blocks = lax.map(one_block, (jnp.arange(block_count, dtype=jnp.int32), query_blocks))
    return (mixed_blocks.reshape(length, W_HEADS * W_DIM), jnp.transpose(log_blocks, (1, 0, 2)).reshape(W_HEADS, length))

def reference(tokens, input_norm_gain, mq_weight, mk_weight, mv_weight, mo_weight, gate_weight, gate_bias, decay_extra, m_gain, aq_weight, ak_weight, av_weight, sink_logit, out_m_weight, out_a_weight):
    length = tokens.shape[0]
    normed = rms_rows(tokens.astype(jnp.float32), input_norm_gain).astype(jnp.bfloat16)

    def project(weight_mat):
        return jnp.dot(normed, weight_mat, preferred_element_type=jnp.float32)
    m_query = stored(project(mq_weight))
    m_key = stored(project(mk_weight))
    m_value = stored(project(mv_weight))
    m_out = stored(project(mo_weight))
    gates = project(gate_weight.reshape(D, 4 * M_HEADS)).reshape(length, 4, M_HEADS) + gate_bias[None]

    def heads_first(matrix):
        return jnp.transpose(matrix.astype(jnp.float32).reshape(length, M_HEADS, M_DIM), (1, 0, 2))
    queries = heads_first(m_query)
    key_vecs = heads_first(m_key) * M_DIM ** (-0.5)
    value_vecs = heads_first(m_value)
    in_fwd = gates[:, 0, :].T
    forget_fwd = jax.nn.log_sigmoid(gates[:, 1, :].T) + decay_extra[0]
    in_bwd = gates[:, 2, :].T
    forget_bwd = jax.nn.log_sigmoid(gates[:, 3, :].T) + decay_extra[1]
    zero_state = (jnp.zeros((M_HEADS, M_DIM, M_DIM), jnp.float32), jnp.zeros((M_HEADS, M_DIM), jnp.float32), jnp.zeros((M_HEADS,), jnp.float32))
    hidden_fwd, forward_unused = block_pass(queries, key_vecs, value_vecs, in_fwd, forget_fwd, zero_state)
    hidden_bwd, unused_bwd = block_pass(flip_tokens(queries), flip_tokens(key_vecs), flip_tokens(value_vecs), flip_tokens(in_bwd), flip_tokens(forget_bwd), zero_state)
    cell_out = hidden_fwd + flip_tokens(hidden_bwd)
    gate_open = jax.nn.sigmoid(m_out.astype(jnp.float32)).reshape(length, M_HEADS, M_DIM)
    cell_rows = jnp.transpose(cell_out, (1, 0, 2)) * gate_open
    mixed_m = rms_rows(cell_rows, m_gain.reshape(M_HEADS, M_DIM)).astype(jnp.bfloat16).reshape(length, M_WIDTH)
    a_query = stored(project(aq_weight))
    a_key = stored(project(ak_weight))
    a_value = stored(project(av_weight))
    mixed_a, log_total = window_attention(a_query, a_key, a_value, sink_logit)
    mixed = jnp.dot(mixed_m, out_m_weight, preferred_element_type=jnp.float32) + jnp.dot(mixed_a, out_a_weight, preferred_element_type=jnp.float32)
    return (mixed.astype(jnp.bfloat16), log_total)
```

```python
import functools

import jax
import jax.numpy as jnp
from jax import lax
from jax.experimental import pallas as pl
from jax.experimental.pallas import tpu as pltpu
from jax.sharding import PartitionSpec as P

M_DIM = 128
W_DIM = 64
WINDOW = 128
STATE_ROWS = 136


EPS = 1e-06
FLOOR_LOG = -1e30
HIGHEST = lax.Precision.HIGHEST
MESH = pl.DeviceIdType.MESH


def rms_rows(inputs, gain_vec):
    return inputs * lax.rsqrt(jnp.mean(inputs * inputs, axis=-1, keepdims=True) + EPS) * gain_vec


def stored(result):
    return lax.optimization_barrier(result.astype(jnp.bfloat16))


def remote(src, dst, send_sem, recv_sem, **where):
    return pltpu.make_async_remote_copy(
        src_ref=src,
        dst_ref=dst,
        send_sem=send_sem,
        recv_sem=recv_sem,
        device_id=where,
        device_id_type=MESH,
    )


def greet(peers):
    barrier = pltpu.get_barrier_semaphore()
    for peer in peers:
        pl.semaphore_signal(barrier, inc=1, device_id=peer, device_id_type=MESH)
    pl.semaphore_wait(barrier, len(peers))


def gather_kernel(
    n,
    g,
    w_ref,
    gt_ref,
    dec_ref,
    tok_ref,
    w_out,
    gt_out,
    dec_out,
    tok_out,
    own_sem,
    in_send,
    in_recv,
    tok_send,
    tok_recv,
    dec_send,
    dec_recv,
    gt_send,
    gt_recv,
    line_send,
    line_recv,
):
    me = lax.axis_index("sp")
    ng = n // g
    q = lax.div(me, g)
    h = lax.rem(me, g)
    greet([{"sp": lax.rem(me + k, n)} for k in range(1, n)])

    def row(k, d):
        return (q + k) * g + lax.rem(h - d + g, g)

    inner = []
    for d in range(1, g):
        to = lax.rem(h + d, g)
        copy = remote(
            w_ref.at[to], w_out.at[me], in_send.at[d - 1], in_recv.at[d - 1], sp=q * g + to
        )
        copy.start()
        inner.append(copy)

    def up(k, d):
        src = w_ref.at[h] if k == 0 and d == 0 else w_out.at[row(-k, d)]
        return remote(
            src,
            w_out.at[row(-k, d)],
            line_send.at[0, k, d],
            line_recv.at[0, k, d],
            sp=me + g,
        )

    def down(k, d):
        src = w_ref.at[h] if k == 0 and d == 0 else w_out.at[row(k, d)]
        return remote(
            src,
            w_out.at[row(k, d)],
            line_send.at[1, k, d],
            line_recv.at[1, k, d],
            sp=me - g,
        )

    def came_up(k, d):
        ref = w_out.at[row(-k, d)]
        return remote(ref, ref, line_send.at[0, k - 1, d], line_recv.at[0, k - 1, d], sp=me)

    def came_down(k, d):
        ref = w_out.at[row(k, d)]
        return remote(ref, ref, line_send.at[1, k - 1, d], line_recv.at[1, k - 1, d], sp=me)

    others = []
    for k in range(ng):
        for d in range(g):
            if k == 0 and d > 0:
                inner[d - 1].wait_recv()
            if k > 0:

                @pl.when(q >= k)
                def _():
                    came_up(k, d).wait_recv()

                @pl.when(q + k < ng)
                def _():
                    came_down(k, d).wait_recv()

            if k < ng - 1:

                @pl.when((q < ng - 1) & (q >= k))
                def _():
                    up(k, d).start()

                @pl.when((q > 0) & (q + k < ng))
                def _():
                    down(k, d).start()

            if k == 0 and d == 0:
                own = [
                    pltpu.make_async_copy(w_ref.at[h], w_out.at[me], own_sem.at[0]),
                    pltpu.make_async_copy(gt_ref.at[h], gt_out.at[me], own_sem.at[1]),
                    pltpu.make_async_copy(dec_ref.at[h], dec_out.at[h], own_sem.at[2]),
                    pltpu.make_async_copy(tok_ref, tok_out.at[h], own_sem.at[3]),
                ]
                for copy in own:
                    copy.start()
                for j in range(1, n):
                    peer = lax.rem(me + j, n)
                    copy = remote(
                        gt_ref.at[lax.rem(peer, g)],
                        gt_out.at[me],
                        gt_send.at[j - 1],
                        gt_recv.at[j - 1],
                        sp=peer,
                    )
                    copy.start()
                    others.append(copy)
                for j in range(1, g):
                    to = lax.rem(h + j, g)
                    copy = remote(
                        dec_ref.at[to],
                        dec_out.at[h],
                        dec_send.at[j - 1],
                        dec_recv.at[j - 1],
                        sp=q * g + to,
                    )
                    copy.start()
                    others.append(copy)
                    copy = remote(
                        tok_ref,
                        tok_out.at[h],
                        tok_send.at[j - 1],
                        tok_recv.at[j - 1],
                        sp=q * g + to,
                    )
                    copy.start()
                    others.append(copy)

    for k in range(ng - 1):
        for d in range(g):

            @pl.when((q < ng - 1) & (q >= k))
            def _():
                up(k, d).wait_send()

            @pl.when((q > 0) & (q + k < ng))
            def _():
                down(k, d).wait_send()

    for copy in inner:
        copy.wait_send()
    for copy in others:
        copy.wait()
    for copy in own:
        copy.wait()


def gather_inputs(n, g, packed, gates_t, decay, normed):
    vmem = pl.BlockSpec(memory_space=pltpu.VMEM)
    hbm = pl.BlockSpec(memory_space=pl.ANY)
    dma = pltpu.SemaphoreType.DMA
    few, ng = max(g - 1, 1), n // g
    return pl.pallas_call(
        functools.partial(gather_kernel, n, g),
        name="gather_inputs",
        out_shape=(
            jax.ShapeDtypeStruct((n,) + packed.shape[1:], packed.dtype),
            jax.ShapeDtypeStruct((n,) + gates_t.shape[1:], gates_t.dtype),
            jax.ShapeDtypeStruct(decay.shape, decay.dtype),
            jax.ShapeDtypeStruct((g,) + normed.shape, normed.dtype),
        ),
        in_specs=[vmem] * 4,
        out_specs=(hbm,) * 4,
        scratch_shapes=[
            dma((4,)),
            dma((few,)),
            dma((few,)),
            dma((few,)),
            dma((few,)),
            dma((few,)),
            dma((few,)),
            dma((n - 1,)),
            dma((n - 1,)),
            dma((2, ng, g)),
            dma((2, ng, g)),
        ],
        compiler_params=pltpu.CompilerParams(collective_id=0, has_side_effects=True),
        cost_estimate=pl.CostEstimate(
            flops=0, bytes_accessed=100_000_000, transcendentals=0
        ),
    )(packed, gates_t, decay, normed)


def state_kernel(
    ng, g, st_ref, kv_ref, st_out, kv_out, up_send, up_recv, dn_send, dn_recv, kv_send, kv_recv
):
    me = lax.axis_index("sp")
    q = lax.div(me, g)
    greet([{"sp": lax.rem(me + k * g, ng * g)} for k in range(1, ng)])
    rows = kv_ref.shape[0]

    def up(k):
        return remote(st_ref.at[0], st_out.at[q], up_send.at[k], up_recv.at[k], sp=me + k * g)

    def down(k):
        return remote(st_ref.at[1], st_out.at[q], dn_send.at[k], dn_recv.at[k], sp=me - k * g)

    def came_up(k):
        return remote(st_ref.at[0], st_out.at[q - k], up_send.at[k], up_recv.at[k], sp=me)

    def came_down(k):
        return remote(st_ref.at[1], st_out.at[q + k], dn_send.at[k], dn_recv.at[k], sp=me)

    def edge(side, peer):
        src = kv_ref.at[pl.ds(rows - WINDOW if side == 0 else 0, WINDOW)]
        return remote(src, kv_out.at[side], kv_send.at[side], kv_recv.at[side], sp=peer)

    if ng > 1:

        @pl.when(q < ng - 1)
        def _():
            edge(0, me + g).start()

        @pl.when(q > 0)
        def _():
            edge(1, me - g).start()

    for k in range(1, ng):

        @pl.when(q + k < ng)
        def _():
            up(k).start()

        @pl.when(q >= k)
        def _():
            down(k).start()

    for k in range(1, ng):

        @pl.when(q + k < ng)
        def _():
            up(k).wait_send()
            came_down(k).wait_recv()

        @pl.when(q >= k)
        def _():
            down(k).wait_send()
            came_up(k).wait_recv()

    if ng > 1:

        @pl.when(q < ng - 1)
        def _():
            edge(0, me + g).wait_send()
            edge(1, me).wait_recv()

        @pl.when(q > 0)
        def _():
            edge(1, me - g).wait_send()
            edge(0, me).wait_recv()


def exchange_states(n, g, states, kv_pairs):
    ng = n // g
    vmem = pl.BlockSpec(memory_space=pltpu.VMEM)
    dma = pltpu.SemaphoreType.DMA
    return pl.pallas_call(
        functools.partial(state_kernel, ng, g),
        name="exchange_states",
        out_shape=(
            jax.ShapeDtypeStruct((ng,) + states.shape[1:], states.dtype),
            jax.ShapeDtypeStruct((2, WINDOW, kv_pairs.shape[1]), kv_pairs.dtype),
        ),
        in_specs=[vmem] * 2,
        out_specs=(vmem,) * 2,
        scratch_shapes=[dma((ng,))] * 4 + [dma((2,))] * 2,
        compiler_params=pltpu.CompilerParams(collective_id=1, has_side_effects=True),
        cost_estimate=pl.CostEstimate(flops=0, bytes_accessed=10_000_000, transcendentals=0),
    )(states, kv_pairs)


def mix_kernel(g, tp, mx_ref, lt_ref, mx_out, lt_out, own_sem, mx_send, mx_recv, lt_send, lt_recv):
    me, c = lax.axis_index("sp"), lax.axis_index("tp")
    q, h = lax.div(me, g), lax.rem(me, g)
    total = g * tp
    mine = h * tp + c
    peers = []
    for k in range(1, total):
        to = lax.rem(mine + k, total)
        peers.append((lax.div(to, tp), lax.rem(to, tp)))
    greet([{"sp": q * g + a, "tp": b} for a, b in peers])
    copies = []
    for k, (a, b) in enumerate(peers):
        copies.append(
            remote(
                mx_ref.at[a], mx_out.at[mine], mx_send.at[k], mx_recv.at[k], sp=q * g + a, tp=b
            )
        )
    for d in range(1, g):
        a = lax.rem(h + d, g)
        copies.append(
            remote(lt_ref.at[a], lt_out.at[h], lt_send.at[d - 1], lt_recv.at[d - 1], sp=q * g + a)
        )
    own = [
        pltpu.make_async_copy(mx_ref.at[h], mx_out.at[mine], own_sem.at[0]),
        pltpu.make_async_copy(lt_ref.at[h], lt_out.at[h], own_sem.at[1]),
    ]
    for copy in copies + own:
        copy.start()
    for copy in copies + own:
        copy.wait()


def exchange_mixed(g, tp, mixed, logs):
    vmem = pl.BlockSpec(memory_space=pltpu.VMEM)
    dma = pltpu.SemaphoreType.DMA
    few, many = max(g - 1, 1), max(g * tp - 1, 1)
    return pl.pallas_call(
        functools.partial(mix_kernel, g, tp),
        name="exchange_mixed",
        out_shape=(
            jax.ShapeDtypeStruct((g * tp,) + mixed.shape[1:], mixed.dtype),
            jax.ShapeDtypeStruct(logs.shape, logs.dtype),
        ),
        in_specs=[vmem] * 2,
        out_specs=(vmem,) * 2,
        scratch_shapes=[dma((2,)), dma((many,)), dma((many,)), dma((few,)), dma((few,))],
        compiler_params=pltpu.CompilerParams(collective_id=2, has_side_effects=True),
        cost_estimate=pl.CostEstimate(flops=0, bytes_accessed=10_000_000, transcendentals=0),
    )(mixed, logs)


def window_attend(a_query, filled_margin, sink_logit, first_row, total_rows):
    tok_rows = a_query.shape[0]
    block_len = WINDOW
    block_count = tok_rows // block_len
    kv_width = filled_margin.shape[1] // 2
    kv_heads = kv_width // W_DIM
    q_heads = a_query.shape[1] // W_DIM
    groups = q_heads // kv_heads
    windows = jnp.concatenate(
        [
            filled_margin[place_idx * block_len : place_idx * block_len + tok_rows].reshape(
                block_count, block_len, 2 * kv_width
            )
            for place_idx in range(3)
        ],
        axis=1,
    )
    key_block = windows[:, :, :kv_width].reshape(block_count, 3 * block_len, kv_heads, W_DIM)
    content_tile = windows[:, :, kv_width:].reshape(block_count, 3 * block_len, kv_heads, W_DIM)
    query_block = a_query.reshape(block_count, block_len, kv_heads, groups, W_DIM)
    scores = jnp.einsum(
        "nqgrd,nkgd->ngrqk", query_block, key_block, preferred_element_type=jnp.float32
    ) * W_DIM ** (-0.5)
    query_off = jnp.arange(block_len, dtype=jnp.int32)
    key_off = jnp.arange(3 * block_len, dtype=jnp.int32) - block_len
    in_window = jnp.abs(query_off[:, None] - key_off[None, :]) <= WINDOW
    key_place = (
        first_row + jnp.arange(block_count, dtype=jnp.int32)[:, None] * block_len + key_off[None, :]
    )
    inside = (key_place >= 0) & (key_place < total_rows)
    usable = in_window[None] & inside[:, None, :]
    scores = jnp.where(usable[:, None, None], scores, -jnp.inf)
    sink_col = sink_logit.reshape(kv_heads, groups)[None, :, :, None]
    peak_log = jnp.maximum(sink_col, jnp.max(scores, axis=-1))
    weights_exp = jnp.exp(scores - peak_log[..., None])
    weight_total_sum = jnp.exp(sink_col - peak_log) + jnp.sum(weights_exp, axis=-1)
    weighted = jnp.einsum(
        "ngrqk,nkgd->nqgrd",
        weights_exp.astype(jnp.bfloat16),
        content_tile,
        preferred_element_type=jnp.float32,
    )
    scale_back = jnp.transpose(weight_total_sum, (0, 3, 1, 2))[..., None]
    mixed_rows = (weighted / scale_back).astype(jnp.bfloat16).reshape(tok_rows, q_heads * W_DIM)
    log_total = jnp.transpose(peak_log + jnp.log(weight_total_sum), (1, 2, 0, 3)).reshape(
        q_heads, tok_rows
    )
    return (mixed_rows, log_total)


def on_device(
    tokens,
    input_norm_gain,
    mq_weight,
    mk_weight,
    mv_weight,
    mo_weight,
    gate_weight,
    gate_bias,
    decay_extra,
    m_gain,
    aq_weight,
    ak_weight,
    av_weight,
    sink_logit,
    out_m_weight,
    out_a_weight,
):
    n, tp = lax.axis_size("sp"), lax.axis_size("tp")
    tok_rows = tokens.shape[0]
    local_heads = gate_weight.shape[2]
    g = 1
    while local_heads % (2 * g) == 0 and n % (2 * g) == 0 and ak_weight.shape[1] % (2 * g * W_DIM) == 0:
        g *= 2
    ng, heads = n // g, local_heads // g
    own = lax.axis_index("sp")
    q, h = lax.div(own, g), lax.rem(own, g)
    rows = mq_weight.shape[0]
    length = g * tok_rows

    normed = rms_rows(tokens.astype(jnp.float32), input_norm_gain).astype(jnp.bfloat16)
    weights = (mq_weight, mk_weight, mv_weight, mo_weight, aq_weight, ak_weight, av_weight)
    packed = jnp.concatenate([w.reshape(rows, g, -1) for w in weights], axis=2)
    packed = jnp.transpose(packed, (1, 0, 2))
    gates_t = jnp.transpose(gate_weight.reshape(rows, 4, g, heads), (2, 1, 3, 0))
    gates_t = gates_t.reshape(g, 4 * heads, rows)
    gates_t = jnp.pad(gates_t, ((0, 0), (0, -(4 * heads) % 16), (0, 0)))
    decay = jnp.transpose(decay_extra.reshape(2, g, heads, tok_rows), (1, 0, 2, 3))
    decay = decay.reshape(g, 2 * heads, tok_rows)
    decay = jnp.pad(decay, ((0, 0), (0, -(2 * heads) % 8), (0, 0)))

    out_w = jnp.concatenate([out_m_weight, out_a_weight], axis=0)
    out_w = lax.all_gather(out_w, "sp", axis=0, tiled=True)

    w_all, gt_all, dec_all, tok_all = gather_inputs(n, g, packed, gates_t, decay, normed)
    tok_all = tok_all.reshape(length, -1)
    w_all = w_all.reshape(n * rows, -1)
    widths = [w.shape[1] // g for w in weights]
    starts = [sum(widths[:i]) for i in range(len(widths) + 1)]
    projected = stored(jnp.dot(tok_all, w_all, preferred_element_type=jnp.float32))
    m_query, m_key, m_value, m_out, a_query, a_key, a_value = [
        projected[:, a:b] for a, b in zip(starts[:-1], starts[1:])
    ]
    kv_pairs = projected[:, starts[5] :]
    gt_rows = jnp.transpose(gt_all, (0, 2, 1)).reshape(n * rows, -1)
    gates = jnp.dot(tok_all, gt_rows, preferred_element_type=jnp.float32)
    gates = gates[:, : 4 * heads].T.reshape(4, heads, length)
    gates = gates + lax.dynamic_slice_in_dim(gate_bias, h * heads, heads, 1)[:, :, None]
    gates = gates.reshape(4, heads, g, tok_rows)
    decay = jnp.transpose(dec_all[:, : 2 * heads], (1, 0, 2)).reshape(2, heads, g, tok_rows)
    in_gate = jnp.stack([gates[0], gates[2]])
    forget = jax.nn.log_sigmoid(jnp.stack([gates[1], gates[3]])) + decay

    def chunks(matrix):
        return jnp.transpose(matrix.reshape(g, tok_rows, heads, M_DIM), (2, 0, 1, 3))

    queries, keys, values = chunks(m_query), chunks(m_key), chunks(m_value)
    queries32, values32 = queries.astype(jnp.float32), values.astype(jnp.float32)
    keys32 = keys.astype(jnp.float32) * M_DIM ** (-0.5)

    place = jnp.arange(tok_rows, dtype=jnp.int32)
    before = place[:, None] <= place[None, :]
    reach = jnp.stack([before, before.T])
    cum = jnp.einsum("dhcs,dst->dhct", forget, reach.astype(jnp.float32), precision=HIGHEST)
    total = jnp.sum(forget, axis=-1)
    log_end = total[..., None] - cum + in_gate
    peak = jnp.max(log_end, axis=-1)
    w_end = jnp.exp(log_end - peak[..., None])
    faded = w_end[..., None] * keys32[None]
    cells = jnp.einsum("dhcsk,hcsv->dhckv", faded, values32, precision=HIGHEST)
    norms = jnp.sum(faded, axis=3)
    summary = jnp.concatenate([cells, norms[..., None, :]], axis=3)

    at = jnp.arange(g, dtype=jnp.int32)
    later = at[:, None] < at[None, :]
    c_, j_, i_ = at[:, None, None], at[None, :, None], at[None, None, :]
    between = jnp.stack([(j_ < i_) & (i_ < c_), (c_ < i_) & (i_ < j_)]).astype(jnp.float32)
    log_local = peak[:, :, None, :] + jnp.einsum(
        "dcji,dhi->dhcj", between, total, precision=HIGHEST
    )
    local_ok = jnp.stack([later.T, later])[:, None]
    to_end = jnp.stack([later, later.T]).astype(jnp.float32)
    log_group = peak + jnp.einsum("dji,dhi->dhj", to_end, total, precision=HIGHEST)
    group_peak = jnp.max(log_group, axis=-1)
    group_scale = jnp.exp(log_group - group_peak[..., None])
    group_sum = jnp.sum(group_scale[..., None, None] * summary, axis=2)
    group_total = jnp.sum(total, axis=-1)
    logs = jnp.stack([group_peak, group_total], axis=-1)[..., None]
    logs = jnp.broadcast_to(logs, logs.shape[:-1] + (M_DIM,))
    message = jnp.concatenate([group_sum, logs], axis=2)
    message = jnp.pad(message, ((0, 0), (0, 0), (0, STATE_ROWS - message.shape[2]), (0, 0)))
    message = message.reshape(2, heads * STATE_ROWS, M_DIM)

    came, edges = exchange_states(n, g, message, kv_pairs)
    came = came.reshape(ng, heads, STATE_ROWS, M_DIM)
    who = jnp.arange(ng, dtype=jnp.int32)
    came = jnp.where((who != q)[:, None, None, None], came, 0.0)
    outer_sum = came[:, :, : M_DIM + 1]
    outer_peak, outer_total = came[:, :, M_DIM + 1, 0], came[:, :, M_DIM + 2, 0]
    o_, u_ = who[:, None], who[None, :]
    crossed = ((o_ < u_) & (u_ < q)) | ((q < u_) & (u_ < o_))
    log_outer = outer_peak + jnp.einsum(
        "ou,uh->oh", crossed.astype(jnp.float32), outer_total, precision=HIGHEST
    )
    lead = jnp.einsum(
        "dci,dhi->dhc", jnp.stack([later.T, later]).astype(jnp.float32), total, precision=HIGHEST
    )
    log_outer = log_outer.T[None, :, None, :] + lead[..., None]
    outer_ok = jnp.stack([who < q, who > q])[:, None, None, :]
    log_src = jnp.concatenate(
        [
            jnp.where(local_ok, log_local, FLOOR_LOG),
            jnp.where(outer_ok, log_outer, FLOOR_LOG),
        ],
        axis=-1,
    )
    ok = jnp.concatenate(
        [jnp.broadcast_to(local_ok, log_local.shape), jnp.broadcast_to(outer_ok, log_outer.shape)],
        axis=-1,
    )
    in_peak = jnp.max(log_src, axis=-1)
    scale = jnp.where(ok, jnp.exp(log_src - in_peak[..., None]), 0.0)
    state = jnp.sum(scale[..., :g, None, None] * summary[:, :, None], axis=3)
    for o in range(ng):
        state = state + scale[..., g + o, None, None] * outer_sum[o][None, :, None]

    log_w = jnp.where(
        jnp.swapaxes(reach, 1, 2)[:, None, None],
        cum[..., :, None] - cum[..., None, :] + in_gate[..., None, :],
        -jnp.inf,
    )
    log_inter = cum + in_peak[..., None]
    row_max = jnp.maximum(jnp.maximum(log_inter, jnp.max(log_w, axis=-1)), 0.0)
    w_inter = jnp.exp(log_inter - row_max)
    scores = jnp.einsum("hctk,hcsk->hcts", queries, keys, preferred_element_type=jnp.float32)
    scores = (scores * M_DIM ** (-0.5))[None] * jnp.exp(log_w - row_max[..., None])
    numer = jnp.einsum("dhcts,hcsv->dhctv", scores, values32, precision=HIGHEST)
    numer = numer + w_inter[..., None] * jnp.einsum(
        "hctk,dhckv->dhctv", queries32, state[..., :M_DIM, :], precision=HIGHEST
    )
    denom = jnp.sum(scores, axis=-1) + w_inter * jnp.sum(
        queries32[None] * state[..., M_DIM:, :], axis=-1
    )
    parts = numer / jnp.maximum(jnp.abs(denom), jnp.exp(-row_max))[..., None]
    cell_rows = jnp.transpose(parts[0] + parts[1], (1, 2, 0, 3)).reshape(length, heads, M_DIM)
    gate_open = jax.nn.sigmoid(m_out.astype(jnp.float32)).reshape(length, heads, M_DIM)
    gain = lax.dynamic_slice_in_dim(m_gain, h * heads * M_DIM, heads * M_DIM, 0)
    mixed_m = (
        rms_rows(cell_rows * gate_open, gain.reshape(heads, M_DIM))
        .astype(jnp.bfloat16)
        .reshape(length, heads * M_DIM)
    )

    edge_ok = jnp.stack([q > 0, q < ng - 1])[:, None, None]
    edges = jnp.where(edge_ok, edges, jnp.zeros_like(edges))
    margin = jnp.concatenate([edges[0], kv_pairs, edges[1]], axis=0)
    sinks = sink_logit.shape[0] // g
    sink = lax.dynamic_slice_in_dim(sink_logit, h * sinks, sinks, 0)
    mixed_a, log_total = window_attend(a_query, margin, sink, q * length, n * tok_rows)

    both = jnp.concatenate([mixed_m, mixed_a], axis=1).reshape(g, tok_rows, -1)
    logs = jnp.transpose(log_total.reshape(sinks, g, tok_rows), (1, 0, 2))
    logs = jnp.pad(logs, ((0, 0), (0, -sinks % 8), (0, 0)))
    mixed_all, logs_all = exchange_mixed(g, tp, both, logs)
    log_total = logs_all[:, :sinks].reshape(g * sinks, tok_rows)
    mixed_all = mixed_all.reshape(g, tp, tok_rows, -1)
    mixed_all = jnp.transpose(mixed_all, (2, 1, 0, 3))
    m_cols = mixed_m.shape[1]
    full_m = mixed_all[..., :m_cols].reshape(tok_rows, n, -1)
    full_a = mixed_all[..., m_cols:].reshape(tok_rows, n, -1)
    full = jnp.concatenate([full_m, full_a], axis=2).reshape(tok_rows, -1)
    mixed = jnp.dot(full, out_w, preferred_element_type=jnp.float32)
    return (mixed.astype(jnp.bfloat16), log_total)


def solution(mesh):
    in_specs = (
        P("sp", None),
        P(),
        P("sp", "tp"),
        P("sp", "tp"),
        P("sp", "tp"),
        P("sp", "tp"),
        P("sp", None, "tp"),
        P(None, "tp"),
        P(None, "tp", "sp"),
        P("tp"),
        P("sp", "tp"),
        P("sp", "tp"),
        P("sp", "tp"),
        P("tp"),
        P("sp", "tp"),
        P("sp", "tp"),
    )
    out_specs = (P("sp", "tp"), P("tp", "sp"))
    return jax.shard_map(
        on_device, mesh=mesh, in_specs=in_specs, out_specs=out_specs, check_vma=False
    )
```

```python
import functools

import jax
import jax.numpy as jnp
from jax import lax
from jax.experimental import pallas as pl
from jax.experimental.pallas import tpu as pltpu
from jax.sharding import PartitionSpec as P

M_DIM = 128
W_DIM = 64
WINDOW = 128
STATE_ROWS = 136


EPS = 1e-06
FLOOR_LOG = -1e30
HIGHEST = lax.Precision.HIGHEST
MESH = pl.DeviceIdType.MESH


def rms_rows(inputs, gain_vec):
    return inputs * lax.rsqrt(jnp.mean(inputs * inputs, axis=-1, keepdims=True) + EPS) * gain_vec


def stored(result):
    return lax.optimization_barrier(result.astype(jnp.bfloat16))


def remote(src, dst, send_sem, recv_sem, **where):
    return pltpu.make_async_remote_copy(
        src_ref=src,
        dst_ref=dst,
        send_sem=send_sem,
        recv_sem=recv_sem,
        device_id=where,
        device_id_type=MESH,
    )


def greet(peers):
    barrier = pltpu.get_barrier_semaphore()
    for peer in peers:
        pl.semaphore_signal(barrier, inc=1, device_id=peer, device_id_type=MESH)
    pl.semaphore_wait(barrier, len(peers))


def gather_kernel(
    n,
    g,
    w_ref,
    gt_ref,
    dec_ref,
    tok_ref,
    ow_ref,
    w_out,
    gt_out,
    dec_out,
    tok_out,
    ow_out,
    own_sem,
    in_send,
    in_recv,
    tok_send,
    tok_recv,
    dec_send,
    dec_recv,
    gt_send,
    gt_recv,
    line_send,
    line_recv,
    ow_send,
    ow_recv,
):
    me = lax.axis_index("sp")
    ng = n // g
    q = lax.div(me, g)
    h = lax.rem(me, g)
    greet([{"sp": lax.rem(me + k, n)} for k in range(1, n)])

    def row(k, d):
        return (q + k) * g + lax.rem(h - d + g, g)

    inner = []
    for d in range(1, g):
        to = lax.rem(h + d, g)
        copy = remote(
            w_ref.at[to], w_out.at[me], in_send.at[d - 1], in_recv.at[d - 1], sp=q * g + to
        )
        copy.start()
        inner.append(copy)

    def up(k, d):
        src = w_ref.at[h] if k == 0 and d == 0 else w_out.at[row(-k, d)]
        return remote(
            src,
            w_out.at[row(-k, d)],
            line_send.at[0, k, d],
            line_recv.at[0, k, d],
            sp=me + g,
        )

    def down(k, d):
        src = w_ref.at[h] if k == 0 and d == 0 else w_out.at[row(k, d)]
        return remote(
            src,
            w_out.at[row(k, d)],
            line_send.at[1, k, d],
            line_recv.at[1, k, d],
            sp=me - g,
        )

    def came_up(k, d):
        ref = w_out.at[row(-k, d)]
        return remote(ref, ref, line_send.at[0, k - 1, d], line_recv.at[0, k - 1, d], sp=me)

    def came_down(k, d):
        ref = w_out.at[row(k, d)]
        return remote(ref, ref, line_send.at[1, k - 1, d], line_recv.at[1, k - 1, d], sp=me)

    def out_up(k):
        src = ow_ref if k == 0 else ow_out.at[q - k]
        return remote(src, ow_out.at[q - k], ow_send.at[0, k], ow_recv.at[0, k], sp=me + g)

    def out_down(k):
        src = ow_ref if k == 0 else ow_out.at[q + k]
        return remote(src, ow_out.at[q + k], ow_send.at[1, k], ow_recv.at[1, k], sp=me - g)

    def out_came_up(k):
        ref = ow_out.at[q - k]
        return remote(ref, ref, ow_send.at[0, k - 1], ow_recv.at[0, k - 1], sp=me)

    def out_came_down(k):
        ref = ow_out.at[q + k]
        return remote(ref, ref, ow_send.at[1, k - 1], ow_recv.at[1, k - 1], sp=me)

    others = []
    for k in range(ng):
        for d in range(g):
            if k == 0 and d > 0:
                inner[d - 1].wait_recv()
            if k > 0:

                @pl.when(q >= k)
                def _():
                    came_up(k, d).wait_recv()

                @pl.when(q + k < ng)
                def _():
                    came_down(k, d).wait_recv()

            if k < ng - 1:

                @pl.when((q < ng - 1) & (q >= k))
                def _():
                    up(k, d).start()

                @pl.when((q > 0) & (q + k < ng))
                def _():
                    down(k, d).start()

            if d == g - 1:
                if k > 0:

                    @pl.when(q >= k)
                    def _():
                        out_came_up(k).wait_recv()

                    @pl.when(q + k < ng)
                    def _():
                        out_came_down(k).wait_recv()

                if k < ng - 1:

                    @pl.when((q < ng - 1) & (q >= k))
                    def _():
                        out_up(k).start()

                    @pl.when((q > 0) & (q + k < ng))
                    def _():
                        out_down(k).start()

            if k == 0 and d == 0:
                own = [
                    pltpu.make_async_copy(w_ref.at[h], w_out.at[me], own_sem.at[0]),
                    pltpu.make_async_copy(gt_ref.at[h], gt_out.at[me], own_sem.at[1]),
                    pltpu.make_async_copy(dec_ref.at[h], dec_out.at[h], own_sem.at[2]),
                    pltpu.make_async_copy(tok_ref, tok_out.at[h], own_sem.at[3]),
                    pltpu.make_async_copy(ow_ref, ow_out.at[q], own_sem.at[4]),
                ]
                for copy in own:
                    copy.start()
                for j in range(1, n):
                    peer = lax.rem(me + j, n)
                    copy = remote(
                        gt_ref.at[lax.rem(peer, g)],
                        gt_out.at[me],
                        gt_send.at[j - 1],
                        gt_recv.at[j - 1],
                        sp=peer,
                    )
                    copy.start()
                    others.append(copy)
                for j in range(1, g):
                    to = lax.rem(h + j, g)
                    copy = remote(
                        dec_ref.at[to],
                        dec_out.at[h],
                        dec_send.at[j - 1],
                        dec_recv.at[j - 1],
                        sp=q * g + to,
                    )
                    copy.start()
                    others.append(copy)
                    copy = remote(
                        tok_ref,
                        tok_out.at[h],
                        tok_send.at[j - 1],
                        tok_recv.at[j - 1],
                        sp=q * g + to,
                    )
                    copy.start()
                    others.append(copy)

    for k in range(ng - 1):
        for d in range(g):

            @pl.when((q < ng - 1) & (q >= k))
            def _():
                up(k, d).wait_send()

            @pl.when((q > 0) & (q + k < ng))
            def _():
                down(k, d).wait_send()

        @pl.when((q < ng - 1) & (q >= k))
        def _():
            out_up(k).wait_send()

        @pl.when((q > 0) & (q + k < ng))
        def _():
            out_down(k).wait_send()

    for copy in inner:
        copy.wait_send()
    for copy in others:
        copy.wait()
    for copy in own:
        copy.wait()


def gather_inputs(n, g, packed, gates_t, decay, normed, out_w):
    vmem = pl.BlockSpec(memory_space=pltpu.VMEM)
    hbm = pl.BlockSpec(memory_space=pl.ANY)
    dma = pltpu.SemaphoreType.DMA
    few, ng = max(g - 1, 1), n // g
    return pl.pallas_call(
        functools.partial(gather_kernel, n, g),
        name="gather_inputs",
        out_shape=(
            jax.ShapeDtypeStruct((n,) + packed.shape[1:], packed.dtype),
            jax.ShapeDtypeStruct((n,) + gates_t.shape[1:], gates_t.dtype),
            jax.ShapeDtypeStruct(decay.shape, decay.dtype),
            jax.ShapeDtypeStruct((g,) + normed.shape, normed.dtype),
            jax.ShapeDtypeStruct((ng,) + out_w.shape, out_w.dtype),
        ),
        in_specs=[vmem] * 5,
        out_specs=(hbm,) * 5,
        scratch_shapes=[
            dma((5,)),
            dma((few,)),
            dma((few,)),
            dma((few,)),
            dma((few,)),
            dma((few,)),
            dma((few,)),
            dma((n - 1,)),
            dma((n - 1,)),
            dma((2, ng, g)),
            dma((2, ng, g)),
            dma((2, ng)),
            dma((2, ng)),
        ],
        compiler_params=pltpu.CompilerParams(collective_id=0, has_side_effects=True),
        cost_estimate=pl.CostEstimate(
            flops=0, bytes_accessed=100_000_000, transcendentals=0
        ),
    )(packed, gates_t, decay, normed, out_w)


def state_kernel(
    ng, g, st_ref, kv_ref, st_out, kv_out, up_send, up_recv, dn_send, dn_recv, kv_send, kv_recv
):
    me = lax.axis_index("sp")
    q = lax.div(me, g)
    greet([{"sp": lax.rem(me + k * g, ng * g)} for k in range(1, ng)])
    rows = kv_ref.shape[0]

    def up(k):
        return remote(st_ref.at[0], st_out.at[q], up_send.at[k], up_recv.at[k], sp=me + k * g)

    def down(k):
        return remote(st_ref.at[1], st_out.at[q], dn_send.at[k], dn_recv.at[k], sp=me - k * g)

    def came_up(k):
        return remote(st_ref.at[0], st_out.at[q - k], up_send.at[k], up_recv.at[k], sp=me)

    def came_down(k):
        return remote(st_ref.at[1], st_out.at[q + k], dn_send.at[k], dn_recv.at[k], sp=me)

    def edge(side, peer):
        src = kv_ref.at[pl.ds(rows - WINDOW if side == 0 else 0, WINDOW)]
        return remote(src, kv_out.at[side], kv_send.at[side], kv_recv.at[side], sp=peer)

    if ng > 1:

        @pl.when(q < ng - 1)
        def _():
            edge(0, me + g).start()

        @pl.when(q > 0)
        def _():
            edge(1, me - g).start()

    for k in range(1, ng):

        @pl.when(q + k < ng)
        def _():
            up(k).start()

        @pl.when(q >= k)
        def _():
            down(k).start()

    for k in range(1, ng):

        @pl.when(q + k < ng)
        def _():
            up(k).wait_send()
            came_down(k).wait_recv()

        @pl.when(q >= k)
        def _():
            down(k).wait_send()
            came_up(k).wait_recv()

    if ng > 1:

        @pl.when(q < ng - 1)
        def _():
            edge(0, me + g).wait_send()
            edge(1, me).wait_recv()

        @pl.when(q > 0)
        def _():
            edge(1, me - g).wait_send()
            edge(0, me).wait_recv()


def exchange_states(n, g, states, kv_pairs):
    ng = n // g
    vmem = pl.BlockSpec(memory_space=pltpu.VMEM)
    dma = pltpu.SemaphoreType.DMA
    return pl.pallas_call(
        functools.partial(state_kernel, ng, g),
        name="exchange_states",
        out_shape=(
            jax.ShapeDtypeStruct((ng,) + states.shape[1:], states.dtype),
            jax.ShapeDtypeStruct((2, WINDOW, kv_pairs.shape[1]), kv_pairs.dtype),
        ),
        in_specs=[vmem] * 2,
        out_specs=(vmem,) * 2,
        scratch_shapes=[dma((ng,))] * 4 + [dma((2,))] * 2,
        compiler_params=pltpu.CompilerParams(collective_id=1, has_side_effects=True),
        cost_estimate=pl.CostEstimate(flops=0, bytes_accessed=10_000_000, transcendentals=0),
    )(states, kv_pairs)


def mix_kernel(g, tp, mx_ref, lt_ref, mx_out, lt_out, own_sem, mx_send, mx_recv, lt_send, lt_recv):
    me, c = lax.axis_index("sp"), lax.axis_index("tp")
    q, h = lax.div(me, g), lax.rem(me, g)
    total = g * tp
    mine = h * tp + c
    peers = []
    for k in range(1, total):
        to = lax.rem(mine + k, total)
        peers.append((lax.div(to, tp), lax.rem(to, tp)))
    greet([{"sp": q * g + a, "tp": b} for a, b in peers])
    copies = []
    for k, (a, b) in enumerate(peers):
        copies.append(
            remote(
                mx_ref.at[a], mx_out.at[mine], mx_send.at[k], mx_recv.at[k], sp=q * g + a, tp=b
            )
        )
    for d in range(1, g):
        a = lax.rem(h + d, g)
        copies.append(
            remote(lt_ref.at[a], lt_out.at[h], lt_send.at[d - 1], lt_recv.at[d - 1], sp=q * g + a)
        )
    own = [
        pltpu.make_async_copy(mx_ref.at[h], mx_out.at[mine], own_sem.at[0]),
        pltpu.make_async_copy(lt_ref.at[h], lt_out.at[h], own_sem.at[1]),
    ]
    for copy in copies + own:
        copy.start()
    for copy in copies + own:
        copy.wait()


def exchange_mixed(g, tp, mixed, logs):
    vmem = pl.BlockSpec(memory_space=pltpu.VMEM)
    dma = pltpu.SemaphoreType.DMA
    few, many = max(g - 1, 1), max(g * tp - 1, 1)
    return pl.pallas_call(
        functools.partial(mix_kernel, g, tp),
        name="exchange_mixed",
        out_shape=(
            jax.ShapeDtypeStruct((g * tp,) + mixed.shape[1:], mixed.dtype),
            jax.ShapeDtypeStruct(logs.shape, logs.dtype),
        ),
        in_specs=[vmem] * 2,
        out_specs=(vmem,) * 2,
        scratch_shapes=[dma((2,)), dma((many,)), dma((many,)), dma((few,)), dma((few,))],
        compiler_params=pltpu.CompilerParams(collective_id=2, has_side_effects=True),
        cost_estimate=pl.CostEstimate(flops=0, bytes_accessed=10_000_000, transcendentals=0),
    )(mixed, logs)


def window_attend(a_query, filled_margin, sink_logit, first_row, total_rows):
    tok_rows = a_query.shape[0]
    block_len = WINDOW
    block_count = tok_rows // block_len
    kv_width = filled_margin.shape[1] // 2
    kv_heads = kv_width // W_DIM
    q_heads = a_query.shape[1] // W_DIM
    groups = q_heads // kv_heads
    windows = jnp.concatenate(
        [
            filled_margin[place_idx * block_len : place_idx * block_len + tok_rows].reshape(
                block_count, block_len, 2 * kv_width
            )
            for place_idx in range(3)
        ],
        axis=1,
    )
    key_block = windows[:, :, :kv_width].reshape(block_count, 3 * block_len, kv_heads, W_DIM)
    content_tile = windows[:, :, kv_width:].reshape(block_count, 3 * block_len, kv_heads, W_DIM)
    query_block = a_query.reshape(block_count, block_len, kv_heads, groups, W_DIM)
    scores = jnp.einsum(
        "nqgrd,nkgd->ngrqk", query_block, key_block, preferred_element_type=jnp.float32
    ) * W_DIM ** (-0.5)
    query_off = jnp.arange(block_len, dtype=jnp.int32)
    key_off = jnp.arange(3 * block_len, dtype=jnp.int32) - block_len
    in_window = jnp.abs(query_off[:, None] - key_off[None, :]) <= WINDOW
    key_place = (
        first_row + jnp.arange(block_count, dtype=jnp.int32)[:, None] * block_len + key_off[None, :]
    )
    inside = (key_place >= 0) & (key_place < total_rows)
    usable = in_window[None] & inside[:, None, :]
    scores = jnp.where(usable[:, None, None], scores, -jnp.inf)
    sink_col = sink_logit.reshape(kv_heads, groups)[None, :, :, None]
    peak_log = jnp.maximum(sink_col, jnp.max(scores, axis=-1))
    weights_exp = jnp.exp(scores - peak_log[..., None])
    weight_total_sum = jnp.exp(sink_col - peak_log) + jnp.sum(weights_exp, axis=-1)
    weighted = jnp.einsum(
        "ngrqk,nkgd->nqgrd",
        weights_exp.astype(jnp.bfloat16),
        content_tile,
        preferred_element_type=jnp.float32,
    )
    scale_back = jnp.transpose(weight_total_sum, (0, 3, 1, 2))[..., None]
    mixed_rows = (weighted / scale_back).astype(jnp.bfloat16).reshape(tok_rows, q_heads * W_DIM)
    log_total = jnp.transpose(peak_log + jnp.log(weight_total_sum), (1, 2, 0, 3)).reshape(
        q_heads, tok_rows
    )
    return (mixed_rows, log_total)


def on_device(
    tokens,
    input_norm_gain,
    mq_weight,
    mk_weight,
    mv_weight,
    mo_weight,
    gate_weight,
    gate_bias,
    decay_extra,
    m_gain,
    aq_weight,
    ak_weight,
    av_weight,
    sink_logit,
    out_m_weight,
    out_a_weight,
):
    n, tp = lax.axis_size("sp"), lax.axis_size("tp")
    tok_rows = tokens.shape[0]
    local_heads = gate_weight.shape[2]
    g = 1
    while local_heads % (2 * g) == 0 and n % (2 * g) == 0 and ak_weight.shape[1] % (2 * g * W_DIM) == 0:
        g *= 2
    ng, heads = n // g, local_heads // g
    own = lax.axis_index("sp")
    q, h = lax.div(own, g), lax.rem(own, g)
    rows = mq_weight.shape[0]
    length = g * tok_rows

    normed = rms_rows(tokens.astype(jnp.float32), input_norm_gain).astype(jnp.bfloat16)
    weights = (mq_weight, mk_weight, mv_weight, mo_weight, aq_weight, ak_weight, av_weight)
    packed = jnp.stack(
        [
            jnp.concatenate(
                [w[:, j * (w.shape[1] // g) : (j + 1) * (w.shape[1] // g)] for w in weights], axis=1
            )
            for j in range(g)
        ]
    )
    gates_t = jnp.transpose(gate_weight.reshape(rows, 4, g, heads), (2, 1, 3, 0))
    gates_t = gates_t.reshape(g, 4 * heads, rows)
    gates_t = jnp.pad(gates_t, ((0, 0), (0, -(4 * heads) % 16), (0, 0)))
    decay = jnp.transpose(decay_extra.reshape(2, g, heads, tok_rows), (1, 0, 2, 3))
    decay = decay.reshape(g, 2 * heads, tok_rows)
    decay = jnp.pad(decay, ((0, 0), (0, -(2 * heads) % 8), (0, 0)))

    out_w = jnp.concatenate([out_m_weight, out_a_weight], axis=0)
    out_w_rows = out_w.shape[0]

    w_all, gt_all, dec_all, tok_all, out_w = gather_inputs(
        n, g, packed, gates_t, decay, normed, out_w
    )
    if g > 1:
        planes = [[i * g + j for j in range(g)] for i in range(ng)]
        out_w = lax.all_gather(
            out_w.reshape(-1, out_w.shape[2]),
            "sp",
            axis=0,
            axis_index_groups=planes,
            tiled=True,
        )
    out_w = out_w.reshape(n * out_w_rows, -1)
    tok_all = tok_all.reshape(length, -1)
    w_all = w_all.reshape(n * rows, -1)
    widths = [w.shape[1] // g for w in weights]
    starts = [sum(widths[:i]) for i in range(len(widths) + 1)]
    projected = stored(jnp.dot(tok_all, w_all, preferred_element_type=jnp.float32))
    m_query, m_key, m_value, m_out, a_query, a_key, a_value = [
        projected[:, a:b] for a, b in zip(starts[:-1], starts[1:])
    ]
    kv_pairs = projected[:, starts[5] :]
    gt_rows = jnp.transpose(gt_all, (0, 2, 1)).reshape(n * rows, -1)
    gates = jnp.dot(tok_all, gt_rows, preferred_element_type=jnp.float32)
    gates = gates[:, : 4 * heads].T.reshape(4, heads, length)
    gates = gates + lax.dynamic_slice_in_dim(gate_bias, h * heads, heads, 1)[:, :, None]
    gates = gates.reshape(4, heads, g, tok_rows)
    decay = jnp.transpose(dec_all[:, : 2 * heads], (1, 0, 2)).reshape(2, heads, g, tok_rows)
    in_gate = jnp.stack([gates[0], gates[2]])
    forget = jax.nn.log_sigmoid(jnp.stack([gates[1], gates[3]])) + decay

    def chunks(matrix):
        return jnp.transpose(matrix.reshape(g, tok_rows, heads, M_DIM), (2, 0, 1, 3))

    queries, keys, values = chunks(m_query), chunks(m_key), chunks(m_value)
    queries32, values32 = queries.astype(jnp.float32), values.astype(jnp.float32)
    keys32 = keys.astype(jnp.float32) * M_DIM ** (-0.5)

    place = jnp.arange(tok_rows, dtype=jnp.int32)
    before = place[:, None] <= place[None, :]
    reach = jnp.stack([before, before.T])
    cum = jnp.einsum("dhcs,dst->dhct", forget, reach.astype(jnp.float32), precision=HIGHEST)
    total = jnp.sum(forget, axis=-1)
    log_end = total[..., None] - cum + in_gate
    peak = jnp.max(log_end, axis=-1)
    w_end = jnp.exp(log_end - peak[..., None])
    faded = w_end[..., None] * keys32[None]
    cells = jnp.einsum("dhcsk,hcsv->dhckv", faded, values32, precision=HIGHEST)
    norms = jnp.sum(faded, axis=3)
    summary = jnp.concatenate([cells, norms[..., None, :]], axis=3)

    at = jnp.arange(g, dtype=jnp.int32)
    later = at[:, None] < at[None, :]
    c_, j_, i_ = at[:, None, None], at[None, :, None], at[None, None, :]
    between = jnp.stack([(j_ < i_) & (i_ < c_), (c_ < i_) & (i_ < j_)]).astype(jnp.float32)
    log_local = peak[:, :, None, :] + jnp.einsum(
        "dcji,dhi->dhcj", between, total, precision=HIGHEST
    )
    local_ok = jnp.stack([later.T, later])[:, None]
    to_end = jnp.stack([later, later.T]).astype(jnp.float32)
    log_group = peak + jnp.einsum("dji,dhi->dhj", to_end, total, precision=HIGHEST)
    group_peak = jnp.max(log_group, axis=-1)
    group_scale = jnp.exp(log_group - group_peak[..., None])
    group_sum = jnp.sum(group_scale[..., None, None] * summary, axis=2)
    group_total = jnp.sum(total, axis=-1)
    logs = jnp.stack([group_peak, group_total], axis=-1)[..., None]
    logs = jnp.broadcast_to(logs, logs.shape[:-1] + (M_DIM,))
    message = jnp.concatenate([group_sum, logs], axis=2)
    message = jnp.pad(message, ((0, 0), (0, 0), (0, STATE_ROWS - message.shape[2]), (0, 0)))
    message = message.reshape(2, heads * STATE_ROWS, M_DIM)

    came, edges = exchange_states(n, g, message, kv_pairs)
    came = came.reshape(ng, heads, STATE_ROWS, M_DIM)
    who = jnp.arange(ng, dtype=jnp.int32)
    came = jnp.where((who != q)[:, None, None, None], came, 0.0)
    outer_sum = came[:, :, : M_DIM + 1]
    outer_peak, outer_total = came[:, :, M_DIM + 1, 0], came[:, :, M_DIM + 2, 0]
    o_, u_ = who[:, None], who[None, :]
    crossed = ((o_ < u_) & (u_ < q)) | ((q < u_) & (u_ < o_))
    log_outer = outer_peak + jnp.einsum(
        "ou,uh->oh", crossed.astype(jnp.float32), outer_total, precision=HIGHEST
    )
    lead = jnp.einsum(
        "dci,dhi->dhc", jnp.stack([later.T, later]).astype(jnp.float32), total, precision=HIGHEST
    )
    log_outer = log_outer.T[None, :, None, :] + lead[..., None]
    outer_ok = jnp.stack([who < q, who > q])[:, None, None, :]
    log_src = jnp.concatenate(
        [
            jnp.where(local_ok, log_local, FLOOR_LOG),
            jnp.where(outer_ok, log_outer, FLOOR_LOG),
        ],
        axis=-1,
    )
    ok = jnp.concatenate(
        [jnp.broadcast_to(local_ok, log_local.shape), jnp.broadcast_to(outer_ok, log_outer.shape)],
        axis=-1,
    )
    in_peak = jnp.max(log_src, axis=-1)
    scale = jnp.where(ok, jnp.exp(log_src - in_peak[..., None]), 0.0)
    state = jnp.sum(scale[..., :g, None, None] * summary[:, :, None], axis=3)
    for o in range(ng):
        state = state + scale[..., g + o, None, None] * outer_sum[o][None, :, None]

    log_w = jnp.where(
        jnp.swapaxes(reach, 1, 2)[:, None, None],
        cum[..., :, None] - cum[..., None, :] + in_gate[..., None, :],
        -jnp.inf,
    )
    log_inter = cum + in_peak[..., None]
    row_max = jnp.maximum(jnp.maximum(log_inter, jnp.max(log_w, axis=-1)), 0.0)
    w_inter = jnp.exp(log_inter - row_max)
    scores = jnp.einsum("hctk,hcsk->hcts", queries, keys, preferred_element_type=jnp.float32)
    scores = (scores * M_DIM ** (-0.5))[None] * jnp.exp(log_w - row_max[..., None])
    numer = jnp.einsum("dhcts,hcsv->dhctv", scores, values32, precision=HIGHEST)
    numer = numer + w_inter[..., None] * jnp.einsum(
        "hctk,dhckv->dhctv", queries32, state[..., :M_DIM, :], precision=HIGHEST
    )
    denom = jnp.sum(scores, axis=-1) + w_inter * jnp.sum(
        queries32[None] * state[..., M_DIM:, :], axis=-1
    )
    parts = numer / jnp.maximum(jnp.abs(denom), jnp.exp(-row_max))[..., None]
    cell_rows = jnp.transpose(parts[0] + parts[1], (1, 2, 0, 3)).reshape(length, heads, M_DIM)
    gate_open = jax.nn.sigmoid(m_out.astype(jnp.float32)).reshape(length, heads, M_DIM)
    gain = lax.dynamic_slice_in_dim(m_gain, h * heads * M_DIM, heads * M_DIM, 0)
    mixed_m = (
        rms_rows(cell_rows * gate_open, gain.reshape(heads, M_DIM))
        .astype(jnp.bfloat16)
        .reshape(length, heads * M_DIM)
    )

    edge_ok = jnp.stack([q > 0, q < ng - 1])[:, None, None]
    edges = jnp.where(edge_ok, edges, jnp.zeros_like(edges))
    margin = jnp.concatenate([edges[0], kv_pairs, edges[1]], axis=0)
    sinks = sink_logit.shape[0] // g
    sink = lax.dynamic_slice_in_dim(sink_logit, h * sinks, sinks, 0)
    mixed_a, log_total = window_attend(a_query, margin, sink, q * length, n * tok_rows)

    both = jnp.concatenate([mixed_m, mixed_a], axis=1).reshape(g, tok_rows, -1)
    logs = jnp.transpose(log_total.reshape(sinks, g, tok_rows), (1, 0, 2))
    logs = jnp.pad(logs, ((0, 0), (0, -sinks % 8), (0, 0)))
    mixed_all, logs_all = exchange_mixed(g, tp, both, logs)
    log_total = logs_all[:, :sinks].reshape(g * sinks, tok_rows)
    mixed_all = mixed_all.reshape(g, tp, tok_rows, -1)
    mixed_all = jnp.transpose(mixed_all, (2, 1, 0, 3))
    m_cols = mixed_m.shape[1]
    full_m = mixed_all[..., :m_cols].reshape(tok_rows, n, -1)
    full_a = mixed_all[..., m_cols:].reshape(tok_rows, n, -1)
    full = jnp.concatenate([full_m, full_a], axis=2).reshape(tok_rows, ng, g, -1)
    full = jnp.swapaxes(full, 1, 2).reshape(tok_rows, -1)
    mixed = jnp.dot(full, out_w, preferred_element_type=jnp.float32)
    return (mixed.astype(jnp.bfloat16), log_total)


def solution(mesh):
    in_specs = (
        P("sp", None),
        P(),
        P("sp", "tp"),
        P("sp", "tp"),
        P("sp", "tp"),
        P("sp", "tp"),
        P("sp", None, "tp"),
        P(None, "tp"),
        P(None, "tp", "sp"),
        P("tp"),
        P("sp", "tp"),
        P("sp", "tp"),
        P("sp", "tp"),
        P("tp"),
        P("sp", "tp"),
        P("sp", "tp"),
    )
    out_specs = (P("sp", "tp"), P("tp", "sp"))
    return jax.shard_map(
        on_device, mesh=mesh, in_specs=in_specs, out_specs=out_specs, check_vma=False
    )
```

```python
import functools

import jax
import jax.numpy as jnp
from jax import lax
from jax.experimental import pallas as pl
from jax.experimental.pallas import tpu as pltpu
from jax.sharding import PartitionSpec as P

M_DIM = 128
W_DIM = 64
WINDOW = 128
STATE_ROWS = 136


EPS = 1e-06
FLOOR_LOG = -1e30
HIGHEST = lax.Precision.HIGHEST
MESH = pl.DeviceIdType.MESH


def rms_rows(inputs, gain_vec):
    return inputs * lax.rsqrt(jnp.mean(inputs * inputs, axis=-1, keepdims=True) + EPS) * gain_vec


def stored(result):
    return lax.optimization_barrier(result.astype(jnp.bfloat16))


def remote(src, dst, send_sem, recv_sem, **where):
    return pltpu.make_async_remote_copy(
        src_ref=src,
        dst_ref=dst,
        send_sem=send_sem,
        recv_sem=recv_sem,
        device_id=where,
        device_id_type=MESH,
    )


def greet(peers):
    barrier = pltpu.get_barrier_semaphore()
    for peer in peers:
        pl.semaphore_signal(barrier, inc=1, device_id=peer, device_id_type=MESH)
    pl.semaphore_wait(barrier, len(peers))


def gather_kernel(
    n,
    g,
    w_ref,
    gt_ref,
    dec_ref,
    tok_ref,
    ow_ref,
    w_out,
    gt_out,
    dec_out,
    tok_out,
    ow_out,
    own_sem,
    in_send,
    in_recv,
    tok_send,
    tok_recv,
    dec_send,
    dec_recv,
    gt_send,
    gt_recv,
    line_send,
    line_recv,
    ow_send,
    ow_recv,
):
    me = lax.axis_index("sp")
    ng = n // g
    q = lax.div(me, g)
    h = lax.rem(me, g)
    greet([{"sp": lax.rem(me + k, n)} for k in range(1, n)])

    def row(k, d):
        return (q + k) * g + lax.rem(h - d + g, g)

    inner = []
    for d in range(1, g):
        to = lax.rem(h + d, g)
        copy = remote(
            w_ref.at[to], w_out.at[me], in_send.at[d - 1], in_recv.at[d - 1], sp=q * g + to
        )
        copy.start()
        inner.append(copy)

    def up(k, d):
        src = w_ref.at[h] if k == 0 and d == 0 else w_out.at[row(-k, d)]
        return remote(
            src,
            w_out.at[row(-k, d)],
            line_send.at[0, k, d],
            line_recv.at[0, k, d],
            sp=me + g,
        )

    def down(k, d):
        src = w_ref.at[h] if k == 0 and d == 0 else w_out.at[row(k, d)]
        return remote(
            src,
            w_out.at[row(k, d)],
            line_send.at[1, k, d],
            line_recv.at[1, k, d],
            sp=me - g,
        )

    def came_up(k, d):
        ref = w_out.at[row(-k, d)]
        return remote(ref, ref, line_send.at[0, k - 1, d], line_recv.at[0, k - 1, d], sp=me)

    def came_down(k, d):
        ref = w_out.at[row(k, d)]
        return remote(ref, ref, line_send.at[1, k - 1, d], line_recv.at[1, k - 1, d], sp=me)

    def out_up(k):
        src = ow_ref if k == 0 else ow_out.at[q - k]
        return remote(src, ow_out.at[q - k], ow_send.at[0, k], ow_recv.at[0, k], sp=me + g)

    def out_down(k):
        src = ow_ref if k == 0 else ow_out.at[q + k]
        return remote(src, ow_out.at[q + k], ow_send.at[1, k], ow_recv.at[1, k], sp=me - g)

    def out_came_up(k):
        ref = ow_out.at[q - k]
        return remote(ref, ref, ow_send.at[0, k - 1], ow_recv.at[0, k - 1], sp=me)

    def out_came_down(k):
        ref = ow_out.at[q + k]
        return remote(ref, ref, ow_send.at[1, k - 1], ow_recv.at[1, k - 1], sp=me)

    others = []
    for k in range(ng):
        for d in range(g):
            if k == 0 and d > 0:
                inner[d - 1].wait_recv()
            if k > 0:

                @pl.when(q >= k)
                def _():
                    came_up(k, d).wait_recv()

                @pl.when(q + k < ng)
                def _():
                    came_down(k, d).wait_recv()

            if k < ng - 1:

                @pl.when((q < ng - 1) & (q >= k))
                def _():
                    up(k, d).start()

                @pl.when((q > 0) & (q + k < ng))
                def _():
                    down(k, d).start()

            if d == 0:
                if k > 0:

                    @pl.when(q >= k)
                    def _():
                        out_came_up(k).wait_recv()

                    @pl.when(q + k < ng)
                    def _():
                        out_came_down(k).wait_recv()

                if k < ng - 1:

                    @pl.when((q < ng - 1) & (q >= k))
                    def _():
                        out_up(k).start()

                    @pl.when((q > 0) & (q + k < ng))
                    def _():
                        out_down(k).start()

            if k == 0 and d == 0:
                own = [
                    pltpu.make_async_copy(w_ref.at[h], w_out.at[me], own_sem.at[0]),
                    pltpu.make_async_copy(gt_ref.at[h], gt_out.at[me], own_sem.at[1]),
                    pltpu.make_async_copy(dec_ref.at[h], dec_out.at[h], own_sem.at[2]),
                    pltpu.make_async_copy(tok_ref, tok_out.at[h], own_sem.at[3]),
                    pltpu.make_async_copy(ow_ref, ow_out.at[q], own_sem.at[4]),
                ]
                for copy in own:
                    copy.start()
                for j in range(1, n):
                    peer = lax.rem(me + j, n)
                    copy = remote(
                        gt_ref.at[lax.rem(peer, g)],
                        gt_out.at[me],
                        gt_send.at[j - 1],
                        gt_recv.at[j - 1],
                        sp=peer,
                    )
                    copy.start()
                    others.append(copy)
                for j in range(1, g):
                    to = lax.rem(h + j, g)
                    copy = remote(
                        dec_ref.at[to],
                        dec_out.at[h],
                        dec_send.at[j - 1],
                        dec_recv.at[j - 1],
                        sp=q * g + to,
                    )
                    copy.start()
                    others.append(copy)
                    copy = remote(
                        tok_ref,
                        tok_out.at[h],
                        tok_send.at[j - 1],
                        tok_recv.at[j - 1],
                        sp=q * g + to,
                    )
                    copy.start()
                    others.append(copy)

    for k in range(ng - 1):
        for d in range(g):

            @pl.when((q < ng - 1) & (q >= k))
            def _():
                up(k, d).wait_send()

            @pl.when((q > 0) & (q + k < ng))
            def _():
                down(k, d).wait_send()

        @pl.when((q < ng - 1) & (q >= k))
        def _():
            out_up(k).wait_send()

        @pl.when((q > 0) & (q + k < ng))
        def _():
            out_down(k).wait_send()

    for copy in inner:
        copy.wait_send()
    for copy in others:
        copy.wait()
    for copy in own:
        copy.wait()


def gather_inputs(n, g, packed, gates_t, decay, normed, out_w):
    vmem = pl.BlockSpec(memory_space=pltpu.VMEM)
    hbm = pl.BlockSpec(memory_space=pl.ANY)
    dma = pltpu.SemaphoreType.DMA
    few, ng = max(g - 1, 1), n // g
    return pl.pallas_call(
        functools.partial(gather_kernel, n, g),
        name="gather_inputs",
        out_shape=(
            jax.ShapeDtypeStruct((n,) + packed.shape[1:], packed.dtype),
            jax.ShapeDtypeStruct((n,) + gates_t.shape[1:], gates_t.dtype),
            jax.ShapeDtypeStruct(decay.shape, decay.dtype),
            jax.ShapeDtypeStruct((g,) + normed.shape, normed.dtype),
            jax.ShapeDtypeStruct((ng,) + out_w.shape, out_w.dtype),
        ),
        in_specs=[vmem] * 5,
        out_specs=(hbm,) * 5,
        scratch_shapes=[
            dma((5,)),
            dma((few,)),
            dma((few,)),
            dma((few,)),
            dma((few,)),
            dma((few,)),
            dma((few,)),
            dma((n - 1,)),
            dma((n - 1,)),
            dma((2, ng, g)),
            dma((2, ng, g)),
            dma((2, ng)),
            dma((2, ng)),
        ],
        compiler_params=pltpu.CompilerParams(collective_id=0, has_side_effects=True),
        cost_estimate=pl.CostEstimate(
            flops=0, bytes_accessed=100_000_000, transcendentals=0
        ),
    )(packed, gates_t, decay, normed, out_w)


def state_kernel(
    ng, g, st_ref, kv_ref, st_out, kv_out, up_send, up_recv, dn_send, dn_recv, kv_send, kv_recv
):
    me = lax.axis_index("sp")
    q = lax.div(me, g)
    greet([{"sp": lax.rem(me + k * g, ng * g)} for k in range(1, ng)])
    rows = kv_ref.shape[0]

    def up(k):
        return remote(st_ref.at[0], st_out.at[q], up_send.at[k], up_recv.at[k], sp=me + k * g)

    def down(k):
        return remote(st_ref.at[1], st_out.at[q], dn_send.at[k], dn_recv.at[k], sp=me - k * g)

    def came_up(k):
        return remote(st_ref.at[0], st_out.at[q - k], up_send.at[k], up_recv.at[k], sp=me)

    def came_down(k):
        return remote(st_ref.at[1], st_out.at[q + k], dn_send.at[k], dn_recv.at[k], sp=me)

    def edge(side, peer):
        src = kv_ref.at[pl.ds(rows - WINDOW if side == 0 else 0, WINDOW)]
        return remote(src, kv_out.at[side], kv_send.at[side], kv_recv.at[side], sp=peer)

    if ng > 1:

        @pl.when(q < ng - 1)
        def _():
            edge(0, me + g).start()

        @pl.when(q > 0)
        def _():
            edge(1, me - g).start()

    for k in range(1, ng):

        @pl.when(q + k < ng)
        def _():
            up(k).start()

        @pl.when(q >= k)
        def _():
            down(k).start()

    for k in range(1, ng):

        @pl.when(q + k < ng)
        def _():
            up(k).wait_send()
            came_down(k).wait_recv()

        @pl.when(q >= k)
        def _():
            down(k).wait_send()
            came_up(k).wait_recv()

    if ng > 1:

        @pl.when(q < ng - 1)
        def _():
            edge(0, me + g).wait_send()
            edge(1, me).wait_recv()

        @pl.when(q > 0)
        def _():
            edge(1, me - g).wait_send()
            edge(0, me).wait_recv()


def exchange_states(n, g, states, kv_pairs):
    ng = n // g
    vmem = pl.BlockSpec(memory_space=pltpu.VMEM)
    dma = pltpu.SemaphoreType.DMA
    return pl.pallas_call(
        functools.partial(state_kernel, ng, g),
        name="exchange_states",
        out_shape=(
            jax.ShapeDtypeStruct((ng,) + states.shape[1:], states.dtype),
            jax.ShapeDtypeStruct((2, WINDOW, kv_pairs.shape[1]), kv_pairs.dtype),
        ),
        in_specs=[vmem] * 2,
        out_specs=(vmem,) * 2,
        scratch_shapes=[dma((ng,))] * 4 + [dma((2,))] * 2,
        compiler_params=pltpu.CompilerParams(collective_id=1, has_side_effects=True),
        cost_estimate=pl.CostEstimate(flops=0, bytes_accessed=10_000_000, transcendentals=0),
    )(states, kv_pairs)


def mix_kernel(
    g, tp, mx_ref, lt_ref, mx_out, lt_out, own_sem, mx_send, mx_recv, fw_send, fw_recv, lt_send, lt_recv
):
    me, c = lax.axis_index("sp"), lax.axis_index("tp")
    q, h = lax.div(me, g), lax.rem(me, g)
    greet(
        [{"sp": q * g + lax.rem(h + d, g)} for d in range(1, g)]
        + [{"tp": lax.rem(c + e, tp)} for e in range(1, tp)]
    )
    copies, direct = [], []
    for d in range(1, g):
        a = lax.rem(h + d, g)
        direct.append(
            remote(
                mx_ref.at[a],
                mx_out.at[h * tp + c],
                mx_send.at[d - 1],
                mx_recv.at[d - 1],
                sp=q * g + a,
            )
        )
        copies.append(
            remote(lt_ref.at[a], lt_out.at[h], lt_send.at[d - 1], lt_recv.at[d - 1], sp=q * g + a)
        )
    copies.append(pltpu.make_async_copy(mx_ref.at[h], mx_out.at[h * tp + c], own_sem.at[0]))
    copies.append(pltpu.make_async_copy(lt_ref.at[h], lt_out.at[h], own_sem.at[1]))
    for copy in direct:
        copy.start()

    def pass_on(d, e):
        slot = lax.rem(h - d + g, g) * tp + c
        src = mx_ref.at[h] if d == 0 else mx_out.at[slot]
        return remote(
            src,
            mx_out.at[slot],
            fw_send.at[d, e - 1],
            fw_recv.at[d, e - 1],
            tp=lax.rem(c + e, tp),
        )

    for e in range(1, tp):
        copies.append(pass_on(0, e))
    for copy in copies:
        copy.start()
    for d in range(1, g):
        direct[d - 1].wait_recv()
        for e in range(1, tp):
            copy = pass_on(d, e)
            copy.start()
            copies.append(copy)
    for copy in direct:
        copy.wait_send()
    for copy in copies:
        copy.wait()


def exchange_mixed(g, tp, mixed, logs):
    vmem = pl.BlockSpec(memory_space=pltpu.VMEM)
    dma = pltpu.SemaphoreType.DMA
    few, cores = max(g - 1, 1), max(tp - 1, 1)
    return pl.pallas_call(
        functools.partial(mix_kernel, g, tp),
        name="exchange_mixed",
        out_shape=(
            jax.ShapeDtypeStruct((g * tp,) + mixed.shape[1:], mixed.dtype),
            jax.ShapeDtypeStruct(logs.shape, logs.dtype),
        ),
        in_specs=[vmem] * 2,
        out_specs=(vmem,) * 2,
        scratch_shapes=[
            dma((2,)),
            dma((few,)),
            dma((few,)),
            dma((g, cores)),
            dma((g, cores)),
            dma((few,)),
            dma((few,)),
        ],
        compiler_params=pltpu.CompilerParams(collective_id=2, has_side_effects=True),
        cost_estimate=pl.CostEstimate(flops=0, bytes_accessed=10_000_000, transcendentals=0),
    )(mixed, logs)


def window_attend(a_query, filled_margin, sink_logit, first_row, total_rows):
    tok_rows = a_query.shape[0]
    block_len = WINDOW
    block_count = tok_rows // block_len
    kv_width = filled_margin.shape[1] // 2
    kv_heads = kv_width // W_DIM
    q_heads = a_query.shape[1] // W_DIM
    groups = q_heads // kv_heads
    windows = jnp.concatenate(
        [
            filled_margin[place_idx * block_len : place_idx * block_len + tok_rows].reshape(
                block_count, block_len, 2 * kv_width
            )
            for place_idx in range(3)
        ],
        axis=1,
    )
    key_block = windows[:, :, :kv_width].reshape(block_count, 3 * block_len, kv_heads, W_DIM)
    content_tile = windows[:, :, kv_width:].reshape(block_count, 3 * block_len, kv_heads, W_DIM)
    query_block = a_query.reshape(block_count, block_len, kv_heads, groups, W_DIM)
    scores = jnp.einsum(
        "nqgrd,nkgd->ngrqk", query_block, key_block, preferred_element_type=jnp.float32
    ) * W_DIM ** (-0.5)
    query_off = jnp.arange(block_len, dtype=jnp.int32)
    key_off = jnp.arange(3 * block_len, dtype=jnp.int32) - block_len
    in_window = jnp.abs(query_off[:, None] - key_off[None, :]) <= WINDOW
    key_place = (
        first_row + jnp.arange(block_count, dtype=jnp.int32)[:, None] * block_len + key_off[None, :]
    )
    inside = (key_place >= 0) & (key_place < total_rows)
    usable = in_window[None] & inside[:, None, :]
    scores = jnp.where(usable[:, None, None], scores, -jnp.inf)
    sink_col = sink_logit.reshape(kv_heads, groups)[None, :, :, None]
    peak_log = jnp.maximum(sink_col, jnp.max(scores, axis=-1))
    weights_exp = jnp.exp(scores - peak_log[..., None])
    weight_total_sum = jnp.exp(sink_col - peak_log) + jnp.sum(weights_exp, axis=-1)
    weighted = jnp.einsum(
        "ngrqk,nkgd->nqgrd",
        weights_exp.astype(jnp.bfloat16),
        content_tile,
        preferred_element_type=jnp.float32,
    )
    scale_back = jnp.transpose(weight_total_sum, (0, 3, 1, 2))[..., None]
    mixed_rows = (weighted / scale_back).astype(jnp.bfloat16).reshape(tok_rows, q_heads * W_DIM)
    log_total = jnp.transpose(peak_log + jnp.log(weight_total_sum), (1, 2, 0, 3)).reshape(
        q_heads, tok_rows
    )
    return (mixed_rows, log_total)


def on_device(
    tokens,
    input_norm_gain,
    mq_weight,
    mk_weight,
    mv_weight,
    mo_weight,
    gate_weight,
    gate_bias,
    decay_extra,
    m_gain,
    aq_weight,
    ak_weight,
    av_weight,
    sink_logit,
    out_m_weight,
    out_a_weight,
):
    n, tp = lax.axis_size("sp"), lax.axis_size("tp")
    tok_rows = tokens.shape[0]
    local_heads = gate_weight.shape[2]
    g = 1
    while local_heads % (2 * g) == 0 and n % (2 * g) == 0 and ak_weight.shape[1] % (2 * g * W_DIM) == 0:
        g *= 2
    ng, heads = n // g, local_heads // g
    own = lax.axis_index("sp")
    q, h = lax.div(own, g), lax.rem(own, g)
    rows = mq_weight.shape[0]
    length = g * tok_rows

    normed = rms_rows(tokens.astype(jnp.float32), input_norm_gain).astype(jnp.bfloat16)
    weights = (mq_weight, mk_weight, mv_weight, mo_weight, aq_weight, ak_weight, av_weight)
    packed = jnp.stack(
        [
            jnp.concatenate(
                [w[:, j * (w.shape[1] // g) : (j + 1) * (w.shape[1] // g)] for w in weights], axis=1
            )
            for j in range(g)
        ]
    )
    gates_t = jnp.transpose(gate_weight.reshape(rows, 4, g, heads), (2, 1, 3, 0))
    gates_t = gates_t.reshape(g, 4 * heads, rows)
    gates_t = jnp.pad(gates_t, ((0, 0), (0, -(4 * heads) % 16), (0, 0)))
    decay = jnp.transpose(decay_extra.reshape(2, g, heads, tok_rows), (1, 0, 2, 3))
    decay = decay.reshape(g, 2 * heads, tok_rows)
    decay = jnp.pad(decay, ((0, 0), (0, -(2 * heads) % 8), (0, 0)))

    out_w = jnp.concatenate([out_m_weight, out_a_weight], axis=0)
    out_w_rows = out_w.shape[0]

    w_all, gt_all, dec_all, tok_all, out_w = gather_inputs(
        n, g, packed, gates_t, decay, normed, out_w
    )
    if g > 1:
        planes = [[i * g + j for j in range(g)] for i in range(ng)]
        out_w = lax.all_gather(
            out_w.reshape(-1, out_w.shape[2]),
            "sp",
            axis=0,
            axis_index_groups=planes,
            tiled=True,
        )
    out_w = out_w.reshape(n * out_w_rows, -1)
    tok_all = tok_all.reshape(length, -1)
    w_all = w_all.reshape(n * rows, -1)
    widths = [w.shape[1] // g for w in weights]
    starts = [sum(widths[:i]) for i in range(len(widths) + 1)]
    projected = stored(jnp.dot(tok_all, w_all, preferred_element_type=jnp.float32))
    m_query, m_key, m_value, m_out, a_query, a_key, a_value = [
        projected[:, a:b] for a, b in zip(starts[:-1], starts[1:])
    ]
    kv_pairs = projected[:, starts[5] :]
    gt_rows = jnp.transpose(gt_all, (0, 2, 1)).reshape(n * rows, -1)
    gates = jnp.dot(tok_all, gt_rows, preferred_element_type=jnp.float32)
    gates = gates[:, : 4 * heads].T.reshape(4, heads, length)
    gates = gates + lax.dynamic_slice_in_dim(gate_bias, h * heads, heads, 1)[:, :, None]
    gates = gates.reshape(4, heads, g, tok_rows)
    decay = jnp.transpose(dec_all[:, : 2 * heads], (1, 0, 2)).reshape(2, heads, g, tok_rows)
    in_gate = jnp.stack([gates[0], gates[2]])
    forget = jax.nn.log_sigmoid(jnp.stack([gates[1], gates[3]])) + decay

    def chunks(matrix):
        return jnp.transpose(matrix.reshape(g, tok_rows, heads, M_DIM), (2, 0, 1, 3))

    queries, keys, values = chunks(m_query), chunks(m_key), chunks(m_value)
    queries32, values32 = queries.astype(jnp.float32), values.astype(jnp.float32)
    keys32 = keys.astype(jnp.float32) * M_DIM ** (-0.5)

    place = jnp.arange(tok_rows, dtype=jnp.int32)
    before = place[:, None] <= place[None, :]
    reach = jnp.stack([before, before.T])
    cum = jnp.einsum("dhcs,dst->dhct", forget, reach.astype(jnp.float32), precision=HIGHEST)
    total = jnp.sum(forget, axis=-1)
    log_end = total[..., None] - cum + in_gate
    peak = jnp.max(log_end, axis=-1)
    w_end = jnp.exp(log_end - peak[..., None])
    faded = w_end[..., None] * keys32[None]
    cells = jnp.einsum("dhcsk,hcsv->dhckv", faded, values32, precision=HIGHEST)
    norms = jnp.sum(faded, axis=3)
    summary = jnp.concatenate([cells, norms[..., None, :]], axis=3)

    at = jnp.arange(g, dtype=jnp.int32)
    later = at[:, None] < at[None, :]
    c_, j_, i_ = at[:, None, None], at[None, :, None], at[None, None, :]
    between = jnp.stack([(j_ < i_) & (i_ < c_), (c_ < i_) & (i_ < j_)]).astype(jnp.float32)
    log_local = peak[:, :, None, :] + jnp.einsum(
        "dcji,dhi->dhcj", between, total, precision=HIGHEST
    )
    local_ok = jnp.stack([later.T, later])[:, None]
    to_end = jnp.stack([later, later.T]).astype(jnp.float32)
    log_group = peak + jnp.einsum("dji,dhi->dhj", to_end, total, precision=HIGHEST)
    group_peak = jnp.max(log_group, axis=-1)
    group_scale = jnp.exp(log_group - group_peak[..., None])
    group_sum = jnp.sum(group_scale[..., None, None] * summary, axis=2)
    group_total = jnp.sum(total, axis=-1)
    logs = jnp.stack([group_peak, group_total], axis=-1)[..., None]
    logs = jnp.broadcast_to(logs, logs.shape[:-1] + (M_DIM,))
    message = jnp.concatenate([group_sum, logs], axis=2)
    message = jnp.pad(message, ((0, 0), (0, 0), (0, STATE_ROWS - message.shape[2]), (0, 0)))
    message = message.reshape(2, heads * STATE_ROWS, M_DIM)

    came, edges = exchange_states(n, g, message, kv_pairs)
    came = came.reshape(ng, heads, STATE_ROWS, M_DIM)
    who = jnp.arange(ng, dtype=jnp.int32)
    came = jnp.where((who != q)[:, None, None, None], came, 0.0)
    outer_sum = came[:, :, : M_DIM + 1]
    outer_peak, outer_total = came[:, :, M_DIM + 1, 0], came[:, :, M_DIM + 2, 0]
    o_, u_ = who[:, None], who[None, :]
    crossed = ((o_ < u_) & (u_ < q)) | ((q < u_) & (u_ < o_))
    log_outer = outer_peak + jnp.einsum(
        "ou,uh->oh", crossed.astype(jnp.float32), outer_total, precision=HIGHEST
    )
    lead = jnp.einsum(
        "dci,dhi->dhc", jnp.stack([later.T, later]).astype(jnp.float32), total, precision=HIGHEST
    )
    log_outer = log_outer.T[None, :, None, :] + lead[..., None]
    outer_ok = jnp.stack([who < q, who > q])[:, None, None, :]
    log_src = jnp.concatenate(
        [
            jnp.where(local_ok, log_local, FLOOR_LOG),
            jnp.where(outer_ok, log_outer, FLOOR_LOG),
        ],
        axis=-1,
    )
    ok = jnp.concatenate(
        [jnp.broadcast_to(local_ok, log_local.shape), jnp.broadcast_to(outer_ok, log_outer.shape)],
        axis=-1,
    )
    in_peak = jnp.max(log_src, axis=-1)
    scale = jnp.where(ok, jnp.exp(log_src - in_peak[..., None]), 0.0)
    state = jnp.sum(scale[..., :g, None, None] * summary[:, :, None], axis=3)
    for o in range(ng):
        state = state + scale[..., g + o, None, None] * outer_sum[o][None, :, None]

    log_w = jnp.where(
        jnp.swapaxes(reach, 1, 2)[:, None, None],
        cum[..., :, None] - cum[..., None, :] + in_gate[..., None, :],
        -jnp.inf,
    )
    log_inter = cum + in_peak[..., None]
    row_max = jnp.maximum(jnp.maximum(log_inter, jnp.max(log_w, axis=-1)), 0.0)
    w_inter = jnp.exp(log_inter - row_max)
    scores = jnp.einsum("hctk,hcsk->hcts", queries, keys, preferred_element_type=jnp.float32)
    scores = (scores * M_DIM ** (-0.5))[None] * jnp.exp(log_w - row_max[..., None])
    numer = jnp.einsum("dhcts,hcsv->dhctv", scores, values32, precision=HIGHEST)
    numer = numer + w_inter[..., None] * jnp.einsum(
        "hctk,dhckv->dhctv", queries32, state[..., :M_DIM, :], precision=HIGHEST
    )
    denom = jnp.sum(scores, axis=-1) + w_inter * jnp.sum(
        queries32[None] * state[..., M_DIM:, :], axis=-1
    )
    parts = numer / jnp.maximum(jnp.abs(denom), jnp.exp(-row_max))[..., None]
    cell_rows = jnp.transpose(parts[0] + parts[1], (1, 2, 0, 3)).reshape(length, heads, M_DIM)
    gate_open = jax.nn.sigmoid(m_out.astype(jnp.float32)).reshape(length, heads, M_DIM)
    gain = lax.dynamic_slice_in_dim(m_gain, h * heads * M_DIM, heads * M_DIM, 0)
    mixed_m = (
        rms_rows(cell_rows * gate_open, gain.reshape(heads, M_DIM))
        .astype(jnp.bfloat16)
        .reshape(length, heads * M_DIM)
    )

    edge_ok = jnp.stack([q > 0, q < ng - 1])[:, None, None]
    edges = jnp.where(edge_ok, edges, jnp.zeros_like(edges))
    margin = jnp.concatenate([edges[0], kv_pairs, edges[1]], axis=0)
    sinks = sink_logit.shape[0] // g
    sink = lax.dynamic_slice_in_dim(sink_logit, h * sinks, sinks, 0)
    mixed_a, log_total = window_attend(a_query, margin, sink, q * length, n * tok_rows)

    both = jnp.concatenate([mixed_m, mixed_a], axis=1).reshape(g, tok_rows, -1)
    logs = jnp.transpose(log_total.reshape(sinks, g, tok_rows), (1, 0, 2))
    logs = jnp.pad(logs, ((0, 0), (0, -sinks % 8), (0, 0)))
    mixed_all, logs_all = exchange_mixed(g, tp, both, logs)
    log_total = logs_all[:, :sinks].reshape(g * sinks, tok_rows)
    mixed_all = mixed_all.reshape(g, tp, tok_rows, -1)
    mixed_all = jnp.transpose(mixed_all, (2, 1, 0, 3))
    m_cols = mixed_m.shape[1]
    full_m = mixed_all[..., :m_cols].reshape(tok_rows, n, -1)
    full_a = mixed_all[..., m_cols:].reshape(tok_rows, n, -1)
    full = jnp.concatenate([full_m, full_a], axis=2).reshape(tok_rows, ng, g, -1)
    full = jnp.swapaxes(full, 1, 2).reshape(tok_rows, -1)
    mixed = jnp.dot(full, out_w, preferred_element_type=jnp.float32)
    return (mixed.astype(jnp.bfloat16), log_total)


def solution(mesh):
    in_specs = (
        P("sp", None),
        P(),
        P("sp", "tp"),
        P("sp", "tp"),
        P("sp", "tp"),
        P("sp", "tp"),
        P("sp", None, "tp"),
        P(None, "tp"),
        P(None, "tp", "sp"),
        P("tp"),
        P("sp", "tp"),
        P("sp", "tp"),
        P("sp", "tp"),
        P("tp"),
        P("sp", "tp"),
        P("sp", "tp"),
    )
    out_specs = (P("sp", "tp"), P("tp", "sp"))
    return jax.shard_map(
        on_device, mesh=mesh, in_specs=in_specs, out_specs=out_specs, check_vma=False
    )
```
